256 devices in a mesh: grp: 2 (over y), sp: 16 (over z), tp: 8 (over x, core).
Axes of the slice: x: 4, y: 2, z: 16, core: 2. Of those that a mesh axis runs over, the one named last changes fastest.
The devices are a block of a 4x16x16 slice.
Arguments:
- layer_input: bfloat16 [64, 6144, 2048], P(('grp', 'tp'), 'sp'), parts along dimension 0, may hold values from -6 to 6
- input_gain: float32 [2048], replicated, may hold values from 0.1 to 1.9
- key_weight: bfloat16 [2048, 512], replicated, may hold values from -0.125 to 0.125
- value_weight: bfloat16 [2048, 512], replicated, may hold values from -0.125 to 0.125
- stick_offsets: bfloat16 [4, 64, 6144], P(None, ('grp', 'tp'), 'sp'), parts along dimension 1
- head_bias: float32 [16], replicated
- queries: bfloat16 [16, 16, 512], P(('grp', 'tp'), 'sp'), parts along dimension 0, may hold values from -6 to 6
Outputs:
- key_cache: bfloat16 [16, 16, 6144, 128], P(('grp', 'tp'), 'sp'), parts along dimension 0
- value_cache: bfloat16 [16, 16, 6144, 128], P(('grp', 'tp'), 'sp'), parts along dimension 0
- offset_cache: bfloat16 [16, 16, 6144], P(('grp', 'tp'), 'sp'), parts along dimension 0
- first_read: bfloat16 [16, 16, 512], P(('grp', 'tp'), 'sp'), parts along dimension 0
The draws below stay inside these ranges and needn't reach their ends.
There are 2 independent parts, one for each index of `grp`. The reference program is written for one: setup_inputs(seed, part) draws one part's arguments, and reference() takes and returns one part's arrays. A program takes and returns all parts, laid end to end along the dimension named above; an argument that names none is the same for every part. Nothing has to cross between parts.
All inputs are finite; a program needn't handle non-finite values.
Results may differ from the reference program's by a relative error of at most 0.014.
Values may be sent and summed in bfloat16 or wider, within the bound.
No kernel may reach another device: no remote copies, remote signals or barrier semaphores. Data moves between devices by JAX's collectives and lax.ppermute only.
A program may use at most 64 MiB of HBM per device.

```python
import math
import jax
import jax.numpy as jnp
from jax import lax

D = 2048
H = 16
KVH = 4
HD = 128
BLOCK = 384
QG = 4
SEQS = 32
LEN = 6144
N_SP = 16
N_TP = 8


def draw_head_bias(key, part):
    pick_key = jax.random.fold_in(key, 11)
    slow_key = jax.random.fold_in(key, 12)
    fast_key = jax.random.fold_in(key, 13)
    fast_share = 0.5
    fast_heads = jax.random.bernoulli(pick_key, fast_share, (H,))
    slow_value = -math.log(LEN) - jax.random.uniform(slow_key, (H,), jnp.float32, 0.5, 1.5)
    fast_value = -4.0 + jax.random.uniform(fast_key, (H,), jnp.float32, -0.5, 0.5)
    return jnp.where(fast_heads, fast_value, slow_value).astype(jnp.float32)


def draw_stick_offsets(key, part):
    level_key = jax.random.fold_in(key, 21)
    jitter_key = jax.random.fold_in(key, 22)
    place_key = jax.random.fold_in(key, 23)
    height_key = jax.random.fold_in(key, 24)
    level_range = 0.7
    blocks = LEN // BLOCK
    tier_entries = jax.random.uniform(level_key, (KVH, SEQS, blocks), jnp.float32, -level_range, level_range)
    tier_entries = jnp.repeat(tier_entries, BLOCK, axis=2)
    stochastic_jitter = jnp.clip(0.3 * jax.random.normal(jitter_key, (KVH, SEQS, LEN), jnp.float32), -1.0, 1.0)
    slot_destinations = jax.random.randint(place_key, (KVH, SEQS, 2), 0, LEN)
    vertical_extent_entries = math.log(LEN) + jax.random.uniform(height_key, (KVH, SEQS, 2), jnp.float32, 0.0, 1.0)
    sequence_slot_index = jnp.arange(LEN)
    clustered_sets = jnp.sum(jnp.where(sequence_slot_index[None, None, None, :] == slot_destinations[..., None], vertical_extent_entries[..., None], 0.0), axis=2)
    return (tier_entries + stochastic_jitter + clustered_sets).astype(jnp.bfloat16)


def level_of(stream_key, shape, cuts, least, top_value):
    def one(position, blocks):
        steps = jax.random.uniform(jax.random.fold_in(jax.random.fold_in(stream_key, 6), position), (blocks,), jnp.float32, least / len(cuts), top_value / len(cuts))
        return jnp.repeat(jnp.exp(steps), shape[position] // blocks).reshape((-1,) + (1,) * (len(shape) - position - 1))

    loudness = one(*cuts[0])
    for cut in cuts[1:]:
        loudness = loudness * one(*cut)
    return loudness


def normal_values(stream_key, dims, scale, bound, split=(), held_as=jnp.bfloat16):
    entries = jax.random.normal(stream_key, dims, jnp.float32) * scale
    if len(split) > 0:
        entries = level_of(stream_key, dims, split, -0.22, 0.18) * entries
    return jnp.clip(entries, min=-bound, max=bound).astype(held_as)


def setup_inputs(seed: int = 0, part: int = 0) -> dict:
    seeds = jax.random.split(jax.random.key(seed), 8)
    part_splits = jax.random.split(jax.random.fold_in(seeds[7], part), 8)
    return {
        "layer_input": normal_values(part_splits[0], (SEQS, LEN, D), 1.0, 6.0, ((0, 8), (1, 16))),
        "input_gain": jnp.clip(1.0 + 0.18 * jax.random.normal(seeds[1], (D,), jnp.float32), 0.1, 1.9),
        "key_weight": normal_values(seeds[2], (D, KVH * HD), D ** -0.5, 0.125),
        "value_weight": normal_values(seeds[3], (D, KVH * HD), D ** -0.5, 0.125),
        "stick_offsets": draw_stick_offsets(jax.random.fold_in(jax.random.fold_in(seeds[7], part), 71), part),
        "head_bias": draw_head_bias(jax.random.fold_in(seeds[7], 71), part),
        "queries": normal_values(part_splits[6], (N_TP, N_SP, QG * HD), 1.0, 6.0, ((0, 8), (1, 16))),
    }


EPSILON = 1e-06

def rms_scale(matrix):
    return matrix * lax.rsqrt(lax.optimization_barrier(jnp.mean(matrix * matrix, axis=-1, keepdims=True)) + EPSILON)

def stick_weights(scores, spread, carried):
    inside = lax.cumsum(spread, axis=scores.ndim - 1, reverse=True) - spread
    return jnp.exp(jax.nn.log_sigmoid(scores) - inside - carried)

def reference(layer_input, input_gain, key_weight, value_weight, stick_offsets, head_bias, queries):
    group_size = H // KVH
    per_column = N_SP // KVH

    def one_sequence(tokens):
        widened = tokens.astype(jnp.float32)
        normed_rows = (rms_scale(widened) * input_gain).astype(jnp.bfloat16)
        key_rows = jnp.dot(normed_rows, key_weight, preferred_element_type=jnp.float32).astype(jnp.bfloat16)
        value_rows = jnp.dot(normed_rows, value_weight, preferred_element_type=jnp.float32).astype(jnp.bfloat16)
        return (key_rows, value_rows)
    key_rows, value_rows = lax.map(one_sequence, layer_input)
    key_cache = jnp.transpose(key_rows.reshape(N_TP, per_column, LEN, KVH, HD), (0, 1, 3, 2, 4)).reshape(N_TP, N_SP, LEN, HD)
    value_cache = jnp.transpose(value_rows.reshape(N_TP, per_column, LEN, KVH, HD), (0, 1, 3, 2, 4)).reshape(N_TP, N_SP, LEN, HD)
    offset_cache = jnp.transpose(stick_offsets.reshape(KVH, N_TP, per_column, LEN), (1, 2, 0, 3)).reshape(N_TP, N_SP, LEN)
    bias_all = jnp.tile(head_bias.reshape(KVH, group_size), (N_TP * per_column, 1))

    def one_read(pieces):
        query_row, key_block, value_block, offset_row, bias_row = pieces
        scores = jnp.dot(query_row.reshape(group_size, HD), key_block.T, preferred_element_type=jnp.float32)
        scores = scores / math.sqrt(HD) + bias_row[:, None] + offset_row.astype(jnp.float32)[None, :]
        spread = jax.nn.softplus(scores)
        weights = stick_weights(scores, spread, 0.0).astype(jnp.bfloat16)
        mixture = jnp.dot(weights, value_block, preferred_element_type=jnp.float32)
        return rms_scale(mixture).astype(jnp.bfloat16).reshape(group_size * HD)
    first_read = lax.map(one_read, (queries.reshape(N_TP * N_SP, group_size * HD), key_cache.reshape(N_TP * N_SP, LEN, HD), value_cache.reshape(N_TP * N_SP, LEN, HD), offset_cache.reshape(N_TP * N_SP, LEN), bias_all))
    return (key_cache, value_cache, offset_cache, first_read.reshape(N_TP, N_SP, group_size * HD))
```

```python
import functools
import math

import jax
import jax.numpy as jnp
from jax import lax
from jax.experimental import pallas as pl
from jax.experimental.pallas import tpu as pltpu
from jax.sharding import PartitionSpec as P


H = 16
KVH = 4
HD = 128
QG = H // KVH
EPSILON = 1e-06
ROWS = 8

ORDER = tuple((c, k) for c in (2, 1, 3, 0) for k in range(KVH) if c or k)
FIRST = ORDER[0][0]
LATE = 3

ANY = pl.BlockSpec(memory_space=pltpu.HBM)
VMEM = pl.BlockSpec(memory_space=pltpu.VMEM)
SMEM = pl.BlockSpec(memory_space=pltpu.SMEM)


def split_index():
    z = lax.axis_index("sp")
    return lax.div(z, KVH), lax.rem(z, KVH)


def project_kernel(classes, x_ref, gain_ref, key_ref, value_ref, *rest):
    count = len(classes)
    outs = rest[: count * KVH]
    rows, wk, wv, normed, parts, x_sems, w_sems, o_sems = rest[count * KVH :]
    group, member = split_index()
    block_len = x_ref.shape[1]
    loads = [
        pltpu.make_async_copy(x_ref.at[group ^ c], rows.at[n], x_sems.at[n]) for n, c in enumerate(classes)
    ]
    weights = [
        pltpu.make_async_copy(key_ref, wk, w_sems.at[0]),
        pltpu.make_async_copy(value_ref, wv, w_sems.at[1]),
    ]
    loads[0].start()
    weights[0].start()
    weights[1].start()
    for load in loads[1:]:
        load.start()
    gain = gain_ref[...].reshape(1, -1)
    stores = []
    for n in range(count):
        loads[n].wait()
        step = 64

        def normalize(r, _, n=n):
            start = pl.multiple_of(r * step, step)
            wide = rows[n, pl.ds(start, step), :].astype(jnp.float32)
            mean = jnp.mean(wide * wide, axis=-1, keepdims=True)
            normed[pl.ds(start, step), :] = (wide * lax.rsqrt(mean + EPSILON) * gain).astype(jnp.bfloat16)
            return 0

        lax.fori_loop(0, block_len // step, normalize, 0, unroll=True)
        for w, weight in enumerate((wk, wv)):
            if n == 0:
                weights[w].wait()
            product = jnp.dot(normed[...], weight[...], preferred_element_type=jnp.float32).astype(jnp.bfloat16)
            for h in range(KVH):
                parts[n, h, w * block_len : (w + 1) * block_len, :] = product[:, h * HD : (h + 1) * HD]
        for k in range(KVH):
            i = n * KVH + k
            store = pltpu.make_async_copy(parts.at[n, member ^ k], outs[i], o_sems.at[i])
            store.start()
            stores.append(store)
    for store in stores:
        store.wait()


def project(classes, layer_input, input_gain, key_weight, value_weight):
    _, block_len, width = layer_input.shape
    columns = key_weight.shape[1]
    count = len(classes)
    piece = jax.ShapeDtypeStruct((2 * block_len, HD), jnp.bfloat16)
    return pl.pallas_call(
        functools.partial(project_kernel, classes),
        out_shape=[piece] * (count * KVH),
        in_specs=[ANY, VMEM, ANY, ANY],
        out_specs=[ANY] * (count * KVH),
        scratch_shapes=[
            pltpu.VMEM((count, block_len, width), jnp.bfloat16),
            pltpu.VMEM((width, columns), jnp.bfloat16),
            pltpu.VMEM((width, columns), jnp.bfloat16),
            pltpu.VMEM((block_len, width), jnp.bfloat16),
            pltpu.VMEM((count, KVH, 2 * block_len, HD), jnp.bfloat16),
            pltpu.SemaphoreType.DMA((count,)),
            pltpu.SemaphoreType.DMA((2,)),
            pltpu.SemaphoreType.DMA((count * KVH,)),
        ],
        compiler_params=pltpu.CompilerParams(vmem_limit_bytes=48 * 1024 * 1024),
        cost_estimate=pl.CostEstimate(
            flops=4 * count * block_len * width * columns,
            bytes_accessed=count * block_len * width * 2 + 4 * width * columns,
            transcendentals=0,
        ),
        name="project",
    )(layer_input, input_gain, key_weight, value_weight)


def read_kernel(pieces, final, q_ref, bias_ref, offset_ref, *rest):
    count = len(pieces)
    piece_refs = rest[:count]
    rest = rest[count:]
    if final:
        total_in, mixed_in, _, _, key_out, value_out, read_out, totals, mixed = rest[:9]
        rest = rest[9:]
    else:
        key_out, value_out, totals, mixed = rest[:4]
        rest = rest[4:]
    held, scores, in_sems, out_sems = rest
    block_len = held.shape[1] // 2
    group, member = split_index()
    blocks = [(group ^ c) * KVH + (member ^ k) for c, k in pieces]
    loads = [pltpu.make_async_copy(piece_refs[i], held.at[i], in_sems.at[i]) for i in range(count)]
    for load in loads:
        load.start()
    line = lax.broadcasted_iota(jnp.int32, (ROWS, 1), 0)
    bias = jnp.zeros((ROWS, 1), jnp.float32)
    query = jnp.zeros((ROWS, HD), jnp.float32)
    for g in range(QG):
        bias = jnp.where(line == g, bias_ref[member * QG + g], bias)
        query = jnp.where(line == g, q_ref[0, :, g * HD : (g + 1) * HD].astype(jnp.float32), query)
    query = query.astype(jnp.bfloat16)
    if final:
        totals[...] = total_in[...]
        mixed[...] = mixed_in[...]
    stores = []
    for i in range(count):
        loads[i].wait()
        place = pl.ds(pl.multiple_of(blocks[i] * block_len, block_len), block_len)
        for w, out in enumerate((key_out, value_out)):
            store = pltpu.make_async_copy(
                held.at[i, pl.ds(w * block_len, block_len)], out.at[0, 0, place], out_sems.at[2 * i + w]
            )
            store.start()
            stores.append(store)
        found = lax.dot_general(
            query, held[i, :block_len], (((1,), (1,)), ((), ())), preferred_element_type=jnp.float32
        )
        scores[i * ROWS : (i + 1) * ROWS, :] = found / math.sqrt(HD) + bias + offset_ref[pl.ds(blocks[i], 1), :]
    z = scores[...]
    soft = jnp.log1p(jnp.exp(-jnp.abs(z)))
    spread = jnp.maximum(z, 0.0) + soft
    after = (
        lax.broadcasted_iota(jnp.int32, (block_len, block_len), 0)
        > lax.broadcasted_iota(jnp.int32, (block_len, block_len), 1)
    ).astype(jnp.bfloat16)
    high = spread.astype(jnp.bfloat16)
    left = spread - high.astype(jnp.float32)
    middle = left.astype(jnp.bfloat16)
    low = (left - middle.astype(jnp.float32)).astype(jnp.bfloat16)
    inside = (
        jnp.dot(low, after, preferred_element_type=jnp.float32)
        + jnp.dot(middle, after, preferred_element_type=jnp.float32)
        + jnp.dot(high, after, preferred_element_type=jnp.float32)
    )
    weights = jnp.exp(jnp.minimum(z, 0.0) - soft - inside).astype(jnp.bfloat16)
    sums = jnp.sum(spread, axis=-1, keepdims=True)
    for i in range(count):
        lines = slice(i * ROWS, (i + 1) * ROWS)
        totals[blocks[i]] = jnp.broadcast_to(sums[lines], (ROWS, HD))
        mixed[blocks[i]] = jnp.dot(weights[lines], held[i, block_len:], preferred_element_type=jnp.float32)
    if final:
        carried = jnp.zeros((ROWS, HD), jnp.float32)
        mixture = jnp.zeros((ROWS, HD), jnp.float32)
        for block in reversed(range(totals.shape[0])):
            mixture = mixture + jnp.exp(-carried) * mixed[block]
            carried = carried + totals[block]
        mean = jnp.mean(mixture * mixture, axis=-1, keepdims=True)
        read = (mixture * lax.rsqrt(mean + EPSILON)).astype(jnp.bfloat16)
        for g in range(QG):
            read_out[0, :, g * HD : (g + 1) * HD] = read[g : g + 1, :]
    for store in stores:
        store.wait()


def read(pieces, queries, head_bias, offsets, values, earlier=()):
    final = bool(earlier)
    count = len(pieces)
    sp_count, block_len = offsets.shape
    caches = [jax.ShapeDtypeStruct((1, 1, sp_count * block_len, HD), jnp.bfloat16)] * 2
    partial = jax.ShapeDtypeStruct((sp_count, ROWS, HD), jnp.float32)
    scratch = [
        pltpu.VMEM((count, 2 * block_len, HD), jnp.bfloat16),
        pltpu.VMEM((count * ROWS, block_len), jnp.float32),
        pltpu.SemaphoreType.DMA((count,)),
        pltpu.SemaphoreType.DMA((2 * count,)),
    ]
    held = [pltpu.VMEM(partial.shape, partial.dtype)] * 2
    return pl.pallas_call(
        functools.partial(read_kernel, pieces, final),
        out_shape=caches + ([jax.ShapeDtypeStruct(queries.shape, jnp.bfloat16)] if final else [partial] * 2),
        in_specs=[VMEM, SMEM, VMEM] + [ANY] * count + ([VMEM, VMEM, ANY, ANY] if final else []),
        out_specs=[ANY, ANY] + ([VMEM] if final else [VMEM] * 2),
        scratch_shapes=(held if final else []) + scratch,
        input_output_aliases={3 + count + 2: 0, 3 + count + 3: 1} if final else {},
        compiler_params=pltpu.CompilerParams(vmem_limit_bytes=32 * 1024 * 1024),
        cost_estimate=pl.CostEstimate(
            flops=64 * count * block_len * HD, bytes_accessed=8 * count * block_len * HD, transcendentals=0
        ),
        name="read",
    )(queries, head_bias, offsets, *values, *earlier)


def shards(layer_input, input_gain, key_weight, value_weight, stick_offsets, head_bias, queries):
    _, block_len, _ = layer_input.shape
    sp_count = lax.axis_size("sp")
    length = sp_count * block_len
    others = tuple(dict.fromkeys(c for c, _ in ORDER if c != FIRST))

    def pairs(c, k):
        return [(z, ((z // KVH) ^ c) * KVH + ((z % KVH) ^ k)) for z in range(sp_count)]

    args = (layer_input, input_gain, key_weight, value_weight)
    made = {}
    for k, piece in enumerate(project((FIRST,), *args)):
        made[FIRST, k] = piece
    for i, piece in enumerate(project(others, *args)):
        made[others[i // KVH], i % KVH] = piece
    got = {(0, 0): made[0, 0]}
    for c, k in ORDER:
        got[c, k] = lax.ppermute(made[c, k], "sp", pairs(c, k))
    offset_parts = jnp.transpose(stick_offsets, (1, 0, 2)).reshape(sp_count, block_len)
    offset_rows = lax.all_to_all(offset_parts, "sp", split_axis=0, concat_axis=0, tiled=True)
    offset_cache = offset_rows.reshape(1, 1, length)
    offset_rows = offset_rows.astype(jnp.float32)
    early = ((0, 0),) + ORDER[:-LATE]
    late = ORDER[-LATE:]
    key_cache, value_cache, totals, mixed = read(
        early, queries, head_bias, offset_rows, [got[piece] for piece in early]
    )
    key_cache, value_cache, first_read = read(
        late,
        queries,
        head_bias,
        offset_rows,
        [got[piece] for piece in late],
        (totals, mixed, key_cache, value_cache),
    )
    return key_cache, value_cache, offset_cache, first_read


def solution(mesh):
    row = P(("grp", "tp"), "sp", None)
    return jax.shard_map(
        shards,
        mesh=mesh,
        in_specs=(row, P(), P(), P(), P(None, ("grp", "tp"), "sp"), P(), row),
        out_specs=(
            P(("grp", "tp"), "sp", None, None),
            P(("grp", "tp"), "sp", None, None),
            row,
            row,
        ),
        check_vma=False,
    )
```

```python
import functools
import math

import jax
import jax.numpy as jnp
from jax import lax
from jax.experimental import pallas as pl
from jax.experimental.pallas import tpu as pltpu
from jax.sharding import PartitionSpec as P


H = 16
KVH = 4
HD = 128
QG = H // KVH
EPSILON = 1e-06
ROWS = 8
EXTRA = 8

ORDER = tuple((c, k) for c in (2, 1, 3, 0) for k in range(KVH) if c or k)
FIRST = ORDER[0][0]
LATE = 3

ANY = pl.BlockSpec(memory_space=pltpu.HBM)
VMEM = pl.BlockSpec(memory_space=pltpu.VMEM)
SMEM = pl.BlockSpec(memory_space=pltpu.SMEM)


def split_index():
    z = lax.axis_index("sp")
    return lax.div(z, KVH), lax.rem(z, KVH)


def project_kernel(classes, x_ref, gain_ref, key_ref, value_ref, offset_ref, *rest):
    count = len(classes)
    outs = rest[: count * KVH]
    rows, wk, wv, gains, offsets, normed, parts, x_sems, w_sems, o_sems = rest[count * KVH :]
    group, member = split_index()
    block_len = x_ref.shape[1]
    loads = [
        pltpu.make_async_copy(x_ref.at[group ^ c], rows.at[n], x_sems.at[n]) for n, c in enumerate(classes)
    ]
    weights = [
        pltpu.make_async_copy(key_ref, wk, w_sems.at[0]),
        pltpu.make_async_copy(value_ref, wv, w_sems.at[1]),
    ]
    small = [
        pltpu.make_async_copy(gain_ref, gains, w_sems.at[2]),
        pltpu.make_async_copy(offset_ref, offsets, w_sems.at[3]),
    ]
    for load in small:
        load.start()
    loads[0].start()
    weights[0].start()
    weights[1].start()
    for load in loads[1:]:
        load.start()
    for load in small:
        load.wait()
    gain = gains[...].reshape(1, -1)
    line = lax.broadcasted_iota(jnp.int32, (EXTRA, HD), 0)
    prompt = lax.broadcasted_iota(jnp.int32, (x_ref.shape[0], 1), 0)
    for n, c in enumerate(classes):
        for h in range(KVH):
            own = offsets[h].astype(jnp.float32)
            own = jnp.sum(jnp.where(prompt == (group ^ c), own, 0.0), axis=0, keepdims=True)
            extra = jnp.zeros((EXTRA, HD), jnp.float32)
            for j in range(block_len // HD):
                extra = jnp.where(line == j, own[:, j * HD : (j + 1) * HD], extra)
            parts[n, h, 2 * block_len :, :] = extra.astype(jnp.bfloat16)
    stores = []
    for n in range(count):
        loads[n].wait()
        step = 64

        def normalize(r, _, n=n):
            start = pl.multiple_of(r * step, step)
            wide = rows[n, pl.ds(start, step), :].astype(jnp.float32)
            mean = jnp.mean(wide * wide, axis=-1, keepdims=True)
            normed[pl.ds(start, step), :] = (wide * lax.rsqrt(mean + EPSILON) * gain).astype(jnp.bfloat16)
            return 0

        lax.fori_loop(0, block_len // step, normalize, 0, unroll=True)
        for w, weight in enumerate((wk, wv)):
            if n == 0:
                weights[w].wait()
            product = jnp.dot(normed[...], weight[...], preferred_element_type=jnp.float32).astype(jnp.bfloat16)
            for h in range(KVH):
                parts[n, h, w * block_len : (w + 1) * block_len, :] = product[:, h * HD : (h + 1) * HD]
        for k in range(KVH):
            i = n * KVH + k
            store = pltpu.make_async_copy(parts.at[n, member ^ k], outs[i], o_sems.at[i])
            store.start()
            stores.append(store)
    for store in stores:
        store.wait()


def project(classes, layer_input, input_gain, key_weight, value_weight, stick_offsets):
    _, block_len, width = layer_input.shape
    columns = key_weight.shape[1]
    count = len(classes)
    piece = jax.ShapeDtypeStruct((2 * block_len + EXTRA, HD), jnp.bfloat16)
    return pl.pallas_call(
        functools.partial(project_kernel, classes),
        out_shape=[piece] * (count * KVH),
        in_specs=[ANY] * 5,
        out_specs=[ANY] * (count * KVH),
        scratch_shapes=[
            pltpu.VMEM((count, block_len, width), jnp.bfloat16),
            pltpu.VMEM((width, columns), jnp.bfloat16),
            pltpu.VMEM((width, columns), jnp.bfloat16),
            pltpu.VMEM(input_gain.shape, input_gain.dtype),
            pltpu.VMEM(stick_offsets.shape, stick_offsets.dtype),
            pltpu.VMEM((block_len, width), jnp.bfloat16),
            pltpu.VMEM((count, KVH, 2 * block_len + EXTRA, HD), jnp.bfloat16),
            pltpu.SemaphoreType.DMA((count,)),
            pltpu.SemaphoreType.DMA((4,)),
            pltpu.SemaphoreType.DMA((count * KVH,)),
        ],
        compiler_params=pltpu.CompilerParams(vmem_limit_bytes=48 * 1024 * 1024),
        cost_estimate=pl.CostEstimate(
            flops=4 * count * block_len * width * columns,
            bytes_accessed=count * block_len * width * 2 + 4 * width * columns,
            transcendentals=0,
        ),
        name="project",
    )(
        *(
            pltpu.with_memory_space_constraint(value, pltpu.HBM)
            for value in (layer_input, input_gain, key_weight, value_weight, stick_offsets)
        )
    )


def read_kernel(pieces, final, q_ref, bias_ref, *rest):
    count = len(pieces)
    held = rest[:count]
    rest = rest[count:]
    if final:
        total_in, mixed_in, row_in, _, _, key_out, value_out, offset_out, read_out, totals, mixed, rows = rest[:12]
        rest = rest[12:]
    else:
        key_out, value_out, totals, mixed, rows = rest[:5]
        rest = rest[5:]
    scores, out_sems = rest
    block_len = rows.shape[2]
    group, member = split_index()
    blocks = [(group ^ c) * KVH + (member ^ k) for c, k in pieces]
    stores = []
    for i in range(count):
        place = pl.ds(pl.multiple_of(blocks[i] * block_len, block_len), block_len)
        for w, out in enumerate((key_out, value_out)):
            store = pltpu.make_async_copy(
                held[i].at[pl.ds(w * block_len, block_len)], out.at[0, 0, place], out_sems.at[2 * i + w]
            )
            store.start()
            stores.append(store)
    line = lax.broadcasted_iota(jnp.int32, (ROWS, 1), 0)
    bias = jnp.zeros((ROWS, 1), jnp.float32)
    query = jnp.zeros((ROWS, HD), jnp.float32)
    for g in range(QG):
        bias = jnp.where(line == g, bias_ref[member * QG + g], bias)
        query = jnp.where(line == g, q_ref[0, :, g * HD : (g + 1) * HD].astype(jnp.float32), query)
    query = query.astype(jnp.bfloat16)
    if final:
        totals[...] = total_in[...]
        mixed[...] = mixed_in[...]
        rows[...] = row_in[...]
    for i in range(count):
        extra = held[i][2 * block_len :, :].astype(jnp.float32)
        offset = jnp.concatenate([extra[j : j + 1, :] for j in range(block_len // HD)], axis=1)
        rows[blocks[i]] = offset
        found = lax.dot_general(
            query, held[i][:block_len, :], (((1,), (1,)), ((), ())), preferred_element_type=jnp.float32
        )
        scores[i * ROWS : (i + 1) * ROWS, :] = found / math.sqrt(HD) + bias + offset
    z = scores[...]
    soft = jnp.log1p(jnp.exp(-jnp.abs(z)))
    spread = jnp.maximum(z, 0.0) + soft
    after = (
        lax.broadcasted_iota(jnp.int32, (block_len, block_len), 0)
        > lax.broadcasted_iota(jnp.int32, (block_len, block_len), 1)
    ).astype(jnp.bfloat16)
    high = spread.astype(jnp.bfloat16)
    left = spread - high.astype(jnp.float32)
    middle = left.astype(jnp.bfloat16)
    low = (left - middle.astype(jnp.float32)).astype(jnp.bfloat16)
    inside = (
        jnp.dot(low, after, preferred_element_type=jnp.float32)
        + jnp.dot(middle, after, preferred_element_type=jnp.float32)
        + jnp.dot(high, after, preferred_element_type=jnp.float32)
    )
    weights = jnp.exp(jnp.minimum(z, 0.0) - soft - inside).astype(jnp.bfloat16)
    sums = jnp.sum(spread, axis=-1, keepdims=True)
    for i in range(count):
        lines = slice(i * ROWS, (i + 1) * ROWS)
        totals[blocks[i]] = jnp.broadcast_to(sums[lines], (ROWS, HD))
        mixed[blocks[i]] = jnp.dot(
            weights[lines], held[i][block_len : 2 * block_len, :], preferred_element_type=jnp.float32
        )
    if final:
        carried = jnp.zeros((ROWS, HD), jnp.float32)
        mixture = jnp.zeros((ROWS, HD), jnp.float32)
        for block in reversed(range(totals.shape[0])):
            mixture = mixture + jnp.exp(-carried) * mixed[block]
            carried = carried + totals[block]
            offset_out[0, :, block * block_len : (block + 1) * block_len] = rows[block].astype(jnp.bfloat16)
        mean = jnp.mean(mixture * mixture, axis=-1, keepdims=True)
        read = (mixture * lax.rsqrt(mean + EPSILON)).astype(jnp.bfloat16)
        for g in range(QG):
            read_out[0, :, g * HD : (g + 1) * HD] = read[g : g + 1, :]
    for store in stores:
        store.wait()


def read(pieces, queries, head_bias, sp_count, block_len, values, earlier=()):
    final = bool(earlier)
    count = len(pieces)
    length = sp_count * block_len
    caches = [jax.ShapeDtypeStruct((1, 1, length, HD), jnp.bfloat16)] * 2
    partial = [jax.ShapeDtypeStruct((sp_count, ROWS, HD), jnp.float32)] * 2
    partial.append(jax.ShapeDtypeStruct((sp_count, 1, block_len), jnp.float32))
    results = [jax.ShapeDtypeStruct((1, 1, length), jnp.bfloat16), jax.ShapeDtypeStruct(queries.shape, jnp.bfloat16)]
    return pl.pallas_call(
        functools.partial(read_kernel, pieces, final),
        out_shape=caches + (results if final else partial),
        in_specs=[VMEM, SMEM] + [VMEM] * count + ([VMEM, VMEM, VMEM, ANY, ANY] if final else []),
        out_specs=[ANY, ANY] + [VMEM] * (2 if final else 3),
        scratch_shapes=([pltpu.VMEM(p.shape, p.dtype) for p in partial] if final else [])
        + [
            pltpu.VMEM((count * ROWS, block_len), jnp.float32),
            pltpu.SemaphoreType.DMA((2 * count,)),
        ],
        input_output_aliases={2 + count + 3: 0, 2 + count + 4: 1} if final else {},
        compiler_params=pltpu.CompilerParams(vmem_limit_bytes=32 * 1024 * 1024),
        cost_estimate=pl.CostEstimate(
            flops=64 * count * block_len * HD, bytes_accessed=8 * count * block_len * HD, transcendentals=0
        ),
        name="read",
    )(queries, head_bias, *(pltpu.with_memory_space_constraint(value, pltpu.VMEM) for value in values), *earlier)


def shards(layer_input, input_gain, key_weight, value_weight, stick_offsets, head_bias, queries):
    _, block_len, _ = layer_input.shape
    sp_count = lax.axis_size("sp")
    others = tuple(dict.fromkeys(c for c, _ in ORDER if c != FIRST))

    def pairs(c, k):
        return [(z, ((z // KVH) ^ c) * KVH + ((z % KVH) ^ k)) for z in range(sp_count)]

    args = (layer_input, input_gain, key_weight, value_weight, stick_offsets)
    made = {}
    for k, piece in enumerate(project((FIRST,), *args)):
        made[FIRST, k] = piece
    for i, piece in enumerate(project(others, *args)):
        made[others[i // KVH], i % KVH] = piece
    got = {(0, 0): made[0, 0]}
    for c, k in ORDER:
        got[c, k] = lax.ppermute(made[c, k], "sp", pairs(c, k))
    early = ((0, 0),) + ORDER[:-LATE]
    late = ORDER[-LATE:]
    *caches, totals, mixed, rows = read(early, queries, head_bias, sp_count, block_len, [got[piece] for piece in early])
    return tuple(
        read(
            late,
            queries,
            head_bias,
            sp_count,
            block_len,
            [got[piece] for piece in late],
            (totals, mixed, rows, *caches),
        )
    )


def solution(mesh):
    row = P(("grp", "tp"), "sp", None)
    return jax.shard_map(
        shards,
        mesh=mesh,
        in_specs=(row, P(), P(), P(), P(None, ("grp", "tp"), "sp"), P(), row),
        out_specs=(
            P(("grp", "tp"), "sp", None, None),
            P(("grp", "tp"), "sp", None, None),
            row,
            row,
        ),
        check_vma=False,
    )
```

```python
import functools
import math

import jax
import jax.numpy as jnp
from jax import lax
from jax.experimental import pallas as pl
from jax.experimental.pallas import tpu as pltpu
from jax.sharding import PartitionSpec as P


H = 16
KVH = 4
HD = 128
QG = H // KVH
EPSILON = 1e-06
ROWS = 8
EXTRA = 8

ORDER = (
    tuple((2, k) for k in (0, 1, 3, 2))
    + tuple((c, k) for k in (0, 1, 3, 2) for c in (1, 3))
    + tuple((0, k) for k in (1, 3, 2))
)
LEAD = (2,)
FOLLOW = (1, 3, 0)
LATE = 3

ANY = pl.BlockSpec(memory_space=pltpu.HBM)
VMEM = pl.BlockSpec(memory_space=pltpu.VMEM)
SMEM = pl.BlockSpec(memory_space=pltpu.SMEM)


def split_index():
    z = lax.axis_index("sp")
    return lax.div(z, KVH), lax.rem(z, KVH), lax.axis_size("sp") // KVH


def project_kernel(classes, x_ref, gain_ref, key_ref, value_ref, offset_ref, *rest):
    count = len(classes)
    outs = rest[: count * KVH]
    rows, wk, wv, gains, offsets, normed, parts, x_sems, w_sems, o_sems = rest[count * KVH :]
    group, member, groups = split_index()
    prompts = [lax.rem(group + c, groups) for c in classes]
    block_len = x_ref.shape[1]
    loads = [
        pltpu.make_async_copy(x_ref.at[prompts[n]], rows.at[n], x_sems.at[n]) for n in range(count)
    ]
    weights = [
        pltpu.make_async_copy(key_ref, wk, w_sems.at[0]),
        pltpu.make_async_copy(value_ref, wv, w_sems.at[1]),
    ]
    small = [
        pltpu.make_async_copy(gain_ref, gains, w_sems.at[2]),
        pltpu.make_async_copy(offset_ref, offsets, w_sems.at[3]),
    ]
    for load in small:
        load.start()
    loads[0].start()
    weights[0].start()
    weights[1].start()
    for load in loads[1:]:
        load.start()
    for load in small:
        load.wait()
    gain = gains[...].reshape(1, -1)
    line = lax.broadcasted_iota(jnp.int32, (EXTRA, HD), 0)
    prompt = lax.broadcasted_iota(jnp.int32, (x_ref.shape[0], 1), 0)
    for n in range(count):
        for h in range(KVH):
            own = offsets[h].astype(jnp.float32)
            own = jnp.sum(jnp.where(prompt == prompts[n], own, 0.0), axis=0, keepdims=True)
            extra = jnp.zeros((EXTRA, HD), jnp.float32)
            for j in range(block_len // HD):
                extra = jnp.where(line == j, own[:, j * HD : (j + 1) * HD], extra)
            parts[n, h, 2 * block_len :, :] = extra.astype(jnp.bfloat16)
    stores = []
    for n in range(count):
        loads[n].wait()
        step = 64

        def normalize(r, _, n=n):
            start = pl.multiple_of(r * step, step)
            wide = rows[n, pl.ds(start, step), :].astype(jnp.float32)
            mean = jnp.mean(wide * wide, axis=-1, keepdims=True)
            normed[pl.ds(start, step), :] = (wide * lax.rsqrt(mean + EPSILON) * gain).astype(jnp.bfloat16)
            return 0

        lax.fori_loop(0, block_len // step, normalize, 0, unroll=True)
        for w, weight in enumerate((wk, wv)):
            if n == 0:
                weights[w].wait()
            product = jnp.dot(normed[...], weight[...], preferred_element_type=jnp.float32).astype(jnp.bfloat16)
            for h in range(KVH):
                parts[n, h, w * block_len : (w + 1) * block_len, :] = product[:, h * HD : (h + 1) * HD]
        for k in range(KVH):
            i = n * KVH + k
            store = pltpu.make_async_copy(parts.at[n, member ^ k], outs[i], o_sems.at[i])
            store.start()
            stores.append(store)
    for store in stores:
        store.wait()


def project(classes, layer_input, input_gain, key_weight, value_weight, stick_offsets):
    _, block_len, width = layer_input.shape
    columns = key_weight.shape[1]
    count = len(classes)
    piece = jax.ShapeDtypeStruct((2 * block_len + EXTRA, HD), jnp.bfloat16)
    return pl.pallas_call(
        functools.partial(project_kernel, classes),
        out_shape=[piece] * (count * KVH),
        in_specs=[ANY] * 5,
        out_specs=[ANY] * (count * KVH),
        scratch_shapes=[
            pltpu.VMEM((count, block_len, width), jnp.bfloat16),
            pltpu.VMEM((width, columns), jnp.bfloat16),
            pltpu.VMEM((width, columns), jnp.bfloat16),
            pltpu.VMEM(input_gain.shape, input_gain.dtype),
            pltpu.VMEM(stick_offsets.shape, stick_offsets.dtype),
            pltpu.VMEM((block_len, width), jnp.bfloat16),
            pltpu.VMEM((count, KVH, 2 * block_len + EXTRA, HD), jnp.bfloat16),
            pltpu.SemaphoreType.DMA((count,)),
            pltpu.SemaphoreType.DMA((4,)),
            pltpu.SemaphoreType.DMA((count * KVH,)),
        ],
        compiler_params=pltpu.CompilerParams(vmem_limit_bytes=48 * 1024 * 1024),
        cost_estimate=pl.CostEstimate(
            flops=4 * count * block_len * width * columns,
            bytes_accessed=count * block_len * width * 2 + 4 * width * columns,
            transcendentals=0,
        ),
        name="project",
    )(
        *(
            pltpu.with_memory_space_constraint(value, pltpu.HBM)
            for value in (layer_input, input_gain, key_weight, value_weight, stick_offsets)
        )
    )


def read_kernel(pieces, final, q_ref, bias_ref, *rest):
    count = len(pieces)
    held = rest[:count]
    rest = rest[count:]
    if final:
        total_in, mixed_in, row_in, _, _, key_out, value_out, offset_out, read_out, totals, mixed, rows = rest[:12]
        rest = rest[12:]
    else:
        key_out, value_out, totals, mixed, rows = rest[:5]
        rest = rest[5:]
    scores, out_sems = rest
    block_len = rows.shape[2]
    group, member, groups = split_index()
    blocks = [lax.rem(group + groups - c, groups) * KVH + (member ^ k) for c, k in pieces]
    stores = []
    for i in range(count):
        place = pl.ds(pl.multiple_of(blocks[i] * block_len, block_len), block_len)
        for w, out in enumerate((key_out, value_out)):
            store = pltpu.make_async_copy(
                held[i].at[pl.ds(w * block_len, block_len)], out.at[0, 0, place], out_sems.at[2 * i + w]
            )
            store.start()
            stores.append(store)
    line = lax.broadcasted_iota(jnp.int32, (ROWS, 1), 0)
    bias = jnp.zeros((ROWS, 1), jnp.float32)
    query = jnp.zeros((ROWS, HD), jnp.float32)
    for g in range(QG):
        bias = jnp.where(line == g, bias_ref[member * QG + g], bias)
        query = jnp.where(line == g, q_ref[0, :, g * HD : (g + 1) * HD].astype(jnp.float32), query)
    query = query.astype(jnp.bfloat16)
    if final:
        totals[...] = total_in[...]
        mixed[...] = mixed_in[...]
        rows[...] = row_in[...]
    for i in range(count):
        extra = held[i][2 * block_len :, :].astype(jnp.float32)
        offset = jnp.concatenate([extra[j : j + 1, :] for j in range(block_len // HD)], axis=1)
        rows[blocks[i]] = offset
        found = lax.dot_general(
            query, held[i][:block_len, :], (((1,), (1,)), ((), ())), preferred_element_type=jnp.float32
        )
        scores[i * ROWS : (i + 1) * ROWS, :] = found / math.sqrt(HD) + bias + offset
    z = scores[...]
    soft = jnp.log1p(jnp.exp(-jnp.abs(z)))
    spread = jnp.maximum(z, 0.0) + soft
    after = (
        lax.broadcasted_iota(jnp.int32, (block_len, block_len), 0)
        > lax.broadcasted_iota(jnp.int32, (block_len, block_len), 1)
    ).astype(jnp.bfloat16)
    high = spread.astype(jnp.bfloat16)
    left = spread - high.astype(jnp.float32)
    middle = left.astype(jnp.bfloat16)
    low = (left - middle.astype(jnp.float32)).astype(jnp.bfloat16)
    inside = (
        jnp.dot(low, after, preferred_element_type=jnp.float32)
        + jnp.dot(middle, after, preferred_element_type=jnp.float32)
        + jnp.dot(high, after, preferred_element_type=jnp.float32)
    )
    weights = jnp.exp(jnp.minimum(z, 0.0) - soft - inside).astype(jnp.bfloat16)
    sums = jnp.sum(spread, axis=-1, keepdims=True)
    for i in range(count):
        lines = slice(i * ROWS, (i + 1) * ROWS)
        totals[blocks[i]] = jnp.broadcast_to(sums[lines], (ROWS, HD))
        mixed[blocks[i]] = jnp.dot(
            weights[lines], held[i][block_len : 2 * block_len, :], preferred_element_type=jnp.float32
        )
    if final:
        carried = jnp.zeros((ROWS, HD), jnp.float32)
        mixture = jnp.zeros((ROWS, HD), jnp.float32)
        for block in reversed(range(totals.shape[0])):
            mixture = mixture + jnp.exp(-carried) * mixed[block]
            carried = carried + totals[block]
            offset_out[0, :, block * block_len : (block + 1) * block_len] = rows[block].astype(jnp.bfloat16)
        mean = jnp.mean(mixture * mixture, axis=-1, keepdims=True)
        read = (mixture * lax.rsqrt(mean + EPSILON)).astype(jnp.bfloat16)
        for g in range(QG):
            read_out[0, :, g * HD : (g + 1) * HD] = read[g : g + 1, :]
    for store in stores:
        store.wait()


def read(pieces, queries, head_bias, sp_count, block_len, values, earlier=()):
    final = bool(earlier)
    count = len(pieces)
    length = sp_count * block_len
    caches = [jax.ShapeDtypeStruct((1, 1, length, HD), jnp.bfloat16)] * 2
    partial = [jax.ShapeDtypeStruct((sp_count, ROWS, HD), jnp.float32)] * 2
    partial.append(jax.ShapeDtypeStruct((sp_count, 1, block_len), jnp.float32))
    results = [jax.ShapeDtypeStruct((1, 1, length), jnp.bfloat16), jax.ShapeDtypeStruct(queries.shape, jnp.bfloat16)]
    return pl.pallas_call(
        functools.partial(read_kernel, pieces, final),
        out_shape=caches + (results if final else partial),
        in_specs=[VMEM, SMEM] + [VMEM] * count + ([VMEM, VMEM, VMEM, ANY, ANY] if final else []),
        out_specs=[ANY, ANY] + [VMEM] * (2 if final else 3),
        scratch_shapes=([pltpu.VMEM(p.shape, p.dtype) for p in partial] if final else [])
        + [
            pltpu.VMEM((count * ROWS, block_len), jnp.float32),
            pltpu.SemaphoreType.DMA((2 * count,)),
        ],
        input_output_aliases={2 + count + 3: 0, 2 + count + 4: 1} if final else {},
        compiler_params=pltpu.CompilerParams(vmem_limit_bytes=32 * 1024 * 1024),
        cost_estimate=pl.CostEstimate(
            flops=64 * count * block_len * HD, bytes_accessed=8 * count * block_len * HD, transcendentals=0
        ),
        name="read",
    )(queries, head_bias, *(pltpu.with_memory_space_constraint(value, pltpu.VMEM) for value in values), *earlier)


def shards(layer_input, input_gain, key_weight, value_weight, stick_offsets, head_bias, queries):
    _, block_len, _ = layer_input.shape
    sp_count = lax.axis_size("sp")
    groups = sp_count // KVH

    def pairs(c, k):
        return [(z, (z // KVH + c) % groups * KVH + (z % KVH ^ k)) for z in range(sp_count)]

    args = (layer_input, input_gain, key_weight, value_weight, stick_offsets)
    made = {}
    for classes in (LEAD, FOLLOW):
        for i, piece in enumerate(project(classes, *args)):
            made[classes[i // KVH], i % KVH] = piece
    got = {(0, 0): made[0, 0]}
    for c, k in ORDER:
        got[c, k] = lax.ppermute(made[c, k], "sp", pairs(c, k))
    early = ((0, 0),) + ORDER[:-LATE]
    late = ORDER[-LATE:]
    *caches, totals, mixed, rows = read(early, queries, head_bias, sp_count, block_len, [got[piece] for piece in early])
    return tuple(
        read(
            late,
            queries,
            head_bias,
            sp_count,
            block_len,
            [got[piece] for piece in late],
            (totals, mixed, rows, *caches),
        )
    )


def solution(mesh):
    row = P(("grp", "tp"), "sp", None)
    return jax.shard_map(
        shards,
        mesh=mesh,
        in_specs=(row, P(), P(), P(), P(None, ("grp", "tp"), "sp"), P(), row),
        out_specs=(
            P(("grp", "tp"), "sp", None, None),
            P(("grp", "tp"), "sp", None, None),
            row,
            row,
        ),
        check_vma=False,
    )
```

```python
import functools
import math

import jax
import jax.numpy as jnp
from jax import lax
from jax.experimental import pallas as pl
from jax.experimental.pallas import tpu as pltpu
from jax.sharding import PartitionSpec as P


H = 16
KVH = 4
HD = 128
QG = H // KVH
EPSILON = 1e-06
ROWS = 8
EXTRA = 8

ORDER = (
    tuple((2, k) for k in (0, 1, 3, 2))
    + tuple((c, k) for k in (0, 1, 3, 2) for c in (1, 3))
    + tuple((0, k) for k in (1, 3, 2))
)
LEAD = (2,)
FOLLOW = (1, 3, 0)
CHUNKS = 3
STEP = 16
LATE = 3

ANY = pl.BlockSpec(memory_space=pltpu.HBM)
VMEM = pl.BlockSpec(memory_space=pltpu.VMEM)
SMEM = pl.BlockSpec(memory_space=pltpu.SMEM)


def split_index():
    z = lax.axis_index("sp")
    return lax.div(z, KVH), lax.rem(z, KVH), lax.axis_size("sp") // KVH


def project_kernel(classes, heads, given, keep, x_ref, gain_ref, key_ref, value_ref, offset_ref, *rest):
    count = len(classes)
    outs = rest[: count * len(heads)]
    rest = rest[count * len(heads) :]
    normed, *rest = rest
    weights, offsets, w_sems = rest[:3]
    group, member, groups = split_index()
    prompts = [lax.rem(group + c, groups) for c in classes]
    block_len = normed.shape[0] // count
    small = pltpu.make_async_copy(offset_ref, offsets, w_sems.at[2 * len(heads)])
    columns = [pl.ds(pl.multiple_of((member ^ k) * HD, HD), HD) for k in heads]
    loads = [
        pltpu.make_async_copy(ref.at[:, columns[i]], weights.at[i, :, w * HD : (w + 1) * HD], w_sems.at[2 * i + w])
        for i in range(len(heads))
        for w, ref in enumerate((key_ref, value_ref))
    ]
    if not given:
        rows, gains, x_sems = rest[3:]
        gain_load = pltpu.make_async_copy(gain_ref, gains, w_sems.at[2 * len(heads) + 1])
        gain_load.start()
        chunk = block_len // CHUNKS
        reads = [
            pltpu.make_async_copy(
                x_ref.at[prompts[n], pl.ds(i * chunk, chunk)],
                rows.at[pl.ds(n * block_len + i * chunk, chunk)],
                x_sems.at[n * CHUNKS + i],
            )
            for n in range(count)
            for i in range(CHUNKS)
        ]
        for load in reads[:CHUNKS]:
            load.start()
    for load in loads:
        load.start()
    small.start()
    if not given:
        for load in reads[CHUNKS:]:
            load.start()
        gain_load.wait()
        gain = gains[...].reshape(1, -1)
        for i, load in enumerate(reads):
            load.wait()

            def normalize(r, _, i=i):
                start = pl.multiple_of(i * chunk + r * STEP, STEP)
                wide = rows[pl.ds(start, STEP), :].astype(jnp.float32)
                mean = jnp.mean(wide * wide, axis=-1, keepdims=True)
                normed[pl.ds(start, STEP), :] = (wide * lax.rsqrt(mean + EPSILON) * gain).astype(jnp.bfloat16)
                return 0

            lax.fori_loop(0, chunk // STEP, normalize, 0, unroll=True)
    else:
        normed = x_ref
    small.wait()
    line = lax.broadcasted_iota(jnp.int32, (EXTRA, HD), 0)
    prompt = lax.broadcasted_iota(jnp.int32, (offsets.shape[1], 1), 0)
    for n in range(count):
        for i, k in enumerate(heads):
            own = offsets[member ^ k].astype(jnp.float32)
            own = jnp.sum(jnp.where(prompt == prompts[n], own, 0.0), axis=0, keepdims=True)
            extra = jnp.zeros((EXTRA, HD), jnp.float32)
            for j in range(block_len // HD):
                extra = jnp.where(line == j, own[:, j * HD : (j + 1) * HD], extra)
            outs[n * len(heads) + i][2 * block_len :, :] = extra.astype(jnp.bfloat16)
    for i in range(len(heads)):
        loads[2 * i].wait()
        loads[2 * i + 1].wait()
        product = jnp.dot(normed[...], weights[i], preferred_element_type=jnp.float32).astype(jnp.bfloat16)
        for n in range(count):
            out = outs[n * len(heads) + i]
            for w in range(2):
                out[w * block_len : (w + 1) * block_len, :] = product[
                    n * block_len : (n + 1) * block_len, w * HD : (w + 1) * HD
                ]


def project(classes, heads, source, input_gain, key_weight, value_weight, stick_offsets, keep=False):
    given = source.ndim == 2
    width = source.shape[-1]
    block_len = source.shape[-2]
    count = len(classes)
    piece = jax.ShapeDtypeStruct((2 * block_len + EXTRA, HD), jnp.bfloat16)
    normed = (count * block_len, width)
    scratch = [] if keep else [pltpu.VMEM(normed if not given else (block_len, HD), jnp.bfloat16)]
    scratch += [
        pltpu.VMEM((len(heads), width, 2 * HD), jnp.bfloat16),
        pltpu.VMEM(stick_offsets.shape, stick_offsets.dtype),
        pltpu.SemaphoreType.DMA((2 * len(heads) + 2,)),
    ]
    if not given:
        scratch += [
            pltpu.VMEM(normed, jnp.bfloat16),
            pltpu.VMEM(input_gain.shape, input_gain.dtype),
            pltpu.SemaphoreType.DMA((count * CHUNKS,)),
        ]
    made = pl.pallas_call(
        functools.partial(project_kernel, classes, heads, given, keep),
        out_shape=[piece] * (count * len(heads)) + ([jax.ShapeDtypeStruct(normed, jnp.bfloat16)] if keep else []),
        in_specs=[VMEM if given else ANY] + [ANY] * 4,
        out_specs=[VMEM] * (count * len(heads) + keep),
        scratch_shapes=scratch,
        compiler_params=pltpu.CompilerParams(vmem_limit_bytes=48 * 1024 * 1024),
        cost_estimate=pl.CostEstimate(
            flops=4 * count * len(heads) * block_len * width * HD,
            bytes_accessed=count * block_len * width * 2 + 4 * width * HD * len(heads),
            transcendentals=0,
        ),
        name="project",
    )(
        source if given else pltpu.with_memory_space_constraint(source, pltpu.HBM),
        *(
            pltpu.with_memory_space_constraint(value, pltpu.HBM)
            for value in (input_gain, key_weight, value_weight, stick_offsets)
        ),
    )
    pieces = {(c, k): made[n * len(heads) + i] for n, c in enumerate(classes) for i, k in enumerate(heads)}
    return pieces, made[-1]


def read_kernel(pieces, final, q_ref, bias_ref, *rest):
    count = len(pieces)
    held = rest[:count]
    rest = rest[count:]
    if final:
        total_in, mixed_in, row_in, _, _, key_out, value_out, offset_out, read_out, totals, mixed, rows = rest[:12]
        rest = rest[12:]
    else:
        key_out, value_out, totals, mixed, rows = rest[:5]
        rest = rest[5:]
    scores, out_sems = rest
    block_len = rows.shape[2]
    group, member, groups = split_index()
    blocks = [lax.rem(group + groups - c, groups) * KVH + (member ^ k) for c, k in pieces]
    stores = []
    for i in range(count):
        place = pl.ds(pl.multiple_of(blocks[i] * block_len, block_len), block_len)
        for w, out in enumerate((key_out, value_out)):
            store = pltpu.make_async_copy(
                held[i].at[pl.ds(w * block_len, block_len)], out.at[0, 0, place], out_sems.at[2 * i + w]
            )
            store.start()
            stores.append(store)
    line = lax.broadcasted_iota(jnp.int32, (ROWS, 1), 0)
    bias = jnp.zeros((ROWS, 1), jnp.float32)
    query = jnp.zeros((ROWS, HD), jnp.float32)
    for g in range(QG):
        bias = jnp.where(line == g, bias_ref[member * QG + g], bias)
        query = jnp.where(line == g, q_ref[0, :, g * HD : (g + 1) * HD].astype(jnp.float32), query)
    query = query.astype(jnp.bfloat16)
    if final:
        totals[...] = total_in[...]
        mixed[...] = mixed_in[...]
        rows[...] = row_in[...]
    for i in range(count):
        extra = held[i][2 * block_len :, :].astype(jnp.float32)
        offset = jnp.concatenate([extra[j : j + 1, :] for j in range(block_len // HD)], axis=1)
        rows[blocks[i]] = offset
        found = lax.dot_general(
            query, held[i][:block_len, :], (((1,), (1,)), ((), ())), preferred_element_type=jnp.float32
        )
        scores[i * ROWS : (i + 1) * ROWS, :] = found / math.sqrt(HD) + bias + offset
    z = scores[...]
    soft = jnp.log1p(jnp.exp(-jnp.abs(z)))
    spread = jnp.maximum(z, 0.0) + soft
    after = (
        lax.broadcasted_iota(jnp.int32, (HD, HD), 0) > lax.broadcasted_iota(jnp.int32, (HD, HD), 1)
    ).astype(jnp.bfloat16)
    strips = block_len // HD
    lanes = [slice(j * HD, (j + 1) * HD) for j in range(strips)]
    stacked = jnp.concatenate([spread[:, lane] for lane in lanes], axis=0)
    high = stacked.astype(jnp.bfloat16).astype(jnp.float32)
    middle = (stacked - high).astype(jnp.bfloat16).astype(jnp.float32)
    thirds = jnp.concatenate([stacked - high - middle, middle, high], axis=0).astype(jnp.bfloat16)
    found = jnp.dot(thirds, after, preferred_element_type=jnp.float32)
    size = count * ROWS
    found = found[: strips * size] + found[strips * size : 2 * strips * size] + found[2 * strips * size :]
    sums = jnp.zeros((size, 1), jnp.float32)
    parts = []
    for j in reversed(range(strips)):
        inner = found[j * size : (j + 1) * size]
        parts.append(inner + sums)
        sums = sums + inner[:, :1] + spread[:, j * HD : j * HD + 1]
    inside = jnp.concatenate(parts[::-1], axis=1)
    weights = jnp.exp(jnp.minimum(z, 0.0) - soft - inside).astype(jnp.bfloat16)
    for i in range(count):
        lines = slice(i * ROWS, (i + 1) * ROWS)
        totals[blocks[i]] = jnp.broadcast_to(sums[lines], (ROWS, HD))
        mixed[blocks[i]] = jnp.dot(
            weights[lines], held[i][block_len : 2 * block_len, :], preferred_element_type=jnp.float32
        )
    if final:
        carried = jnp.zeros((ROWS, HD), jnp.float32)
        mixture = jnp.zeros((ROWS, HD), jnp.float32)
        for block in reversed(range(totals.shape[0])):
            mixture = mixture + jnp.exp(-carried) * mixed[block]
            carried = carried + totals[block]
            offset_out[0, :, block * block_len : (block + 1) * block_len] = rows[block].astype(jnp.bfloat16)
        mean = jnp.mean(mixture * mixture, axis=-1, keepdims=True)
        read = (mixture * lax.rsqrt(mean + EPSILON)).astype(jnp.bfloat16)
        for g in range(QG):
            read_out[0, :, g * HD : (g + 1) * HD] = read[g : g + 1, :]
    for store in stores:
        store.wait()


def read(pieces, queries, head_bias, sp_count, block_len, values, earlier=()):
    final = bool(earlier)
    count = len(pieces)
    length = sp_count * block_len
    caches = [jax.ShapeDtypeStruct((1, 1, length, HD), jnp.bfloat16)] * 2
    partial = [jax.ShapeDtypeStruct((sp_count, ROWS, HD), jnp.float32)] * 2
    partial.append(jax.ShapeDtypeStruct((sp_count, 1, block_len), jnp.float32))
    results = [jax.ShapeDtypeStruct((1, 1, length), jnp.bfloat16), jax.ShapeDtypeStruct(queries.shape, jnp.bfloat16)]
    return pl.pallas_call(
        functools.partial(read_kernel, pieces, final),
        out_shape=caches + (results if final else partial),
        in_specs=[VMEM, SMEM] + [VMEM] * count + ([VMEM, VMEM, VMEM, ANY, ANY] if final else []),
        out_specs=[ANY, ANY] + [VMEM] * (2 if final else 3),
        scratch_shapes=([pltpu.VMEM(p.shape, p.dtype) for p in partial] if final else [])
        + [
            pltpu.VMEM((count * ROWS, block_len), jnp.float32),
            pltpu.SemaphoreType.DMA((2 * count,)),
        ],
        input_output_aliases={2 + count + 3: 0, 2 + count + 4: 1} if final else {},
        compiler_params=pltpu.CompilerParams(vmem_limit_bytes=32 * 1024 * 1024),
        cost_estimate=pl.CostEstimate(
            flops=64 * count * block_len * HD, bytes_accessed=8 * count * block_len * HD, transcendentals=0
        ),
        name="read",
    )(queries, head_bias, *(pltpu.with_memory_space_constraint(value, pltpu.VMEM) for value in values), *earlier)


def shards(layer_input, input_gain, key_weight, value_weight, stick_offsets, head_bias, queries):
    _, block_len, _ = layer_input.shape
    sp_count = lax.axis_size("sp")
    groups = sp_count // KVH

    def pairs(c, k):
        return [(z, (z // KVH + c) % groups * KVH + (z % KVH ^ k)) for z in range(sp_count)]

    args = (input_gain, key_weight, value_weight, stick_offsets)
    made, normed = project(LEAD, ORDER[0][1:], layer_input, *args, keep=True)
    made.update(project(LEAD, tuple(k for k in range(KVH) if k != ORDER[0][1]), normed, *args)[0])
    made.update(project(FOLLOW, tuple(range(KVH)), layer_input, *args)[0])
    got = {(0, 0): made[0, 0]}
    for c, k in ORDER:
        got[c, k] = lax.ppermute(made[c, k], "sp", pairs(c, k))
    early = ((0, 0),) + ORDER[:-LATE]
    late = ORDER[-LATE:]
    *caches, totals, mixed, rows = read(early, queries, head_bias, sp_count, block_len, [got[piece] for piece in early])
    return tuple(
        read(
            late,
            queries,
            head_bias,
            sp_count,
            block_len,
            [got[piece] for piece in late],
            (totals, mixed, rows, *caches),
        )
    )


def solution(mesh):
    row = P(("grp", "tp"), "sp", None)
    return jax.shard_map(
        shards,
        mesh=mesh,
        in_specs=(row, P(), P(), P(), P(None, ("grp", "tp"), "sp"), P(), row),
        out_specs=(
            P(("grp", "tp"), "sp", None, None),
            P(("grp", "tp"), "sp", None, None),
            row,
            row,
        ),
        check_vma=False,
    )
```

```python
import functools
import math

import jax
import jax.numpy as jnp
from jax import lax
from jax.experimental import pallas as pl
from jax.experimental.pallas import tpu as pltpu
from jax.sharding import PartitionSpec as P


H = 16
KVH = 4
HD = 128
QG = H // KVH
EPSILON = 1e-06
ROWS = 8
EXTRA = 8

ORDER = (
    ((2, 0), (2, 3))
    + ((1, 0), (3, 1), (1, 2), (3, 0))
    + ((2, 2), (2, 1))
    + ((1, 3), (3, 2), (1, 1), (3, 3))
    + ((0, 2), (0, 3), (0, 1))
)
LEAD = (2,)
FOLLOW = (1, 3, 0)
CHUNKS = 3
STEP = 16
LATE = 3

ANY = pl.BlockSpec(memory_space=pltpu.HBM)
VMEM = pl.BlockSpec(memory_space=pltpu.VMEM)
SMEM = pl.BlockSpec(memory_space=pltpu.SMEM)


def split_index():
    z = lax.axis_index("sp")
    return lax.div(z, KVH), lax.rem(z, KVH), lax.axis_size("sp") // KVH


def project_kernel(classes, heads, given, keep, x_ref, gain_ref, key_ref, value_ref, offset_ref, *rest):
    count = len(classes)
    outs = rest[: count * len(heads)]
    rest = rest[count * len(heads) :]
    normed, *rest = rest
    weights, offsets, w_sems = rest[:3]
    group, member, groups = split_index()
    prompts = [lax.rem(group + c, groups) for c in classes]
    block_len = normed.shape[0] // count
    small = pltpu.make_async_copy(offset_ref, offsets, w_sems.at[2 * len(heads)])
    columns = [pl.ds(pl.multiple_of((member ^ k) * HD, HD), HD) for k in heads]
    loads = [
        pltpu.make_async_copy(ref.at[:, columns[i]], weights.at[i, :, w * HD : (w + 1) * HD], w_sems.at[2 * i + w])
        for i in range(len(heads))
        for w, ref in enumerate((key_ref, value_ref))
    ]
    if not given:
        rows, gains, x_sems = rest[3:]
        gain_load = pltpu.make_async_copy(gain_ref, gains, w_sems.at[2 * len(heads) + 1])
        gain_load.start()
        chunk = block_len // CHUNKS
        reads = [
            pltpu.make_async_copy(
                x_ref.at[prompts[n], pl.ds(i * chunk, chunk)],
                rows.at[pl.ds(n * block_len + i * chunk, chunk)],
                x_sems.at[n * CHUNKS + i],
            )
            for n in range(count)
            for i in range(CHUNKS)
        ]
        for load in reads[:CHUNKS]:
            load.start()
    for load in loads:
        load.start()
    small.start()
    if not given:
        for load in reads[CHUNKS:]:
            load.start()
        gain_load.wait()
        gain = gains[...].reshape(1, -1)
        for i, load in enumerate(reads):
            load.wait()

            def normalize(r, _, i=i):
                start = pl.multiple_of(i * chunk + r * STEP, STEP)
                wide = rows[pl.ds(start, STEP), :].astype(jnp.float32)
                mean = jnp.mean(wide * wide, axis=-1, keepdims=True)
                normed[pl.ds(start, STEP), :] = (wide * lax.rsqrt(mean + EPSILON) * gain).astype(jnp.bfloat16)
                return 0

            lax.fori_loop(0, chunk // STEP, normalize, 0, unroll=4)
    else:
        normed = x_ref
    small.wait()
    line = lax.broadcasted_iota(jnp.int32, (EXTRA, HD), 0)
    prompt = lax.broadcasted_iota(jnp.int32, (offsets.shape[1], 1), 0)
    for n in range(count):
        for i, k in enumerate(heads):
            own = offsets[member ^ k].astype(jnp.float32)
            own = jnp.sum(jnp.where(prompt == prompts[n], own, 0.0), axis=0, keepdims=True)
            extra = jnp.zeros((EXTRA, HD), jnp.float32)
            for j in range(block_len // HD):
                extra = jnp.where(line == j, own[:, j * HD : (j + 1) * HD], extra)
            outs[n * len(heads) + i][2 * block_len :, :] = extra.astype(jnp.bfloat16)
    for i in range(len(heads)):
        loads[2 * i].wait()
        loads[2 * i + 1].wait()
        product = jnp.dot(normed[...], weights[i], preferred_element_type=jnp.float32).astype(jnp.bfloat16)
        for n in range(count):
            out = outs[n * len(heads) + i]
            for w in range(2):
                out[w * block_len : (w + 1) * block_len, :] = product[
                    n * block_len : (n + 1) * block_len, w * HD : (w + 1) * HD
                ]


def project(classes, heads, source, input_gain, key_weight, value_weight, stick_offsets, keep=False):
    given = source.ndim == 2
    width = source.shape[-1]
    block_len = source.shape[-2]
    count = len(classes)
    piece = jax.ShapeDtypeStruct((2 * block_len + EXTRA, HD), jnp.bfloat16)
    normed = (count * block_len, width)
    scratch = [] if keep else [pltpu.VMEM(normed if not given else (block_len, HD), jnp.bfloat16)]
    scratch += [
        pltpu.VMEM((len(heads), width, 2 * HD), jnp.bfloat16),
        pltpu.VMEM(stick_offsets.shape, stick_offsets.dtype),
        pltpu.SemaphoreType.DMA((2 * len(heads) + 2,)),
    ]
    if not given:
        scratch += [
            pltpu.VMEM(normed, jnp.bfloat16),
            pltpu.VMEM(input_gain.shape, input_gain.dtype),
            pltpu.SemaphoreType.DMA((count * CHUNKS,)),
        ]
    made = pl.pallas_call(
        functools.partial(project_kernel, classes, heads, given, keep),
        out_shape=[piece] * (count * len(heads)) + ([jax.ShapeDtypeStruct(normed, jnp.bfloat16)] if keep else []),
        in_specs=[VMEM if given else ANY] + [ANY] * 4,
        out_specs=[VMEM] * (count * len(heads) + keep),
        scratch_shapes=scratch,
        compiler_params=pltpu.CompilerParams(vmem_limit_bytes=48 * 1024 * 1024),
        cost_estimate=pl.CostEstimate(
            flops=4 * count * len(heads) * block_len * width * HD,
            bytes_accessed=count * block_len * width * 2 + 4 * width * HD * len(heads),
            transcendentals=0,
        ),
        name="project",
    )(
        source if given else pltpu.with_memory_space_constraint(source, pltpu.HBM),
        *(
            pltpu.with_memory_space_constraint(value, pltpu.HBM)
            for value in (input_gain, key_weight, value_weight, stick_offsets)
        ),
    )
    pieces = {(c, k): made[n * len(heads) + i] for n, c in enumerate(classes) for i, k in enumerate(heads)}
    return pieces, made[-1]


def read_kernel(pieces, final, q_ref, bias_ref, *rest):
    count = len(pieces)
    held = rest[:count]
    rest = rest[count:]
    if final:
        total_in, mixed_in, row_in, _, _, key_out, value_out, offset_out, read_out, totals, mixed, rows = rest[:12]
        rest = rest[12:]
    else:
        key_out, value_out, totals, mixed, rows = rest[:5]
        rest = rest[5:]
    scores, out_sems = rest
    block_len = rows.shape[2]
    group, member, groups = split_index()
    blocks = [lax.rem(group + groups - c, groups) * KVH + (member ^ k) for c, k in pieces]
    stores = []
    for i in range(count):
        place = pl.ds(pl.multiple_of(blocks[i] * block_len, block_len), block_len)
        for w, out in enumerate((key_out, value_out)):
            store = pltpu.make_async_copy(
                held[i].at[pl.ds(w * block_len, block_len)], out.at[0, 0, place], out_sems.at[2 * i + w]
            )
            store.start()
            stores.append(store)
    line = lax.broadcasted_iota(jnp.int32, (ROWS, 1), 0)
    bias = jnp.zeros((ROWS, 1), jnp.float32)
    query = jnp.zeros((ROWS, HD), jnp.float32)
    for g in range(QG):
        bias = jnp.where(line == g, bias_ref[member * QG + g], bias)
        query = jnp.where(line == g, q_ref[0, :, g * HD : (g + 1) * HD].astype(jnp.float32), query)
    query = query.astype(jnp.bfloat16)
    if final:
        totals[...] = total_in[...]
        mixed[...] = mixed_in[...]
        rows[...] = row_in[...]
    for i in range(count):
        extra = held[i][2 * block_len :, :].astype(jnp.float32)
        offset = jnp.concatenate([extra[j : j + 1, :] for j in range(block_len // HD)], axis=1)
        rows[blocks[i]] = offset
        found = lax.dot_general(
            query, held[i][:block_len, :], (((1,), (1,)), ((), ())), preferred_element_type=jnp.float32
        )
        scores[i * ROWS : (i + 1) * ROWS, :] = found / math.sqrt(HD) + bias + offset
    z = scores[...]
    soft = jnp.log1p(jnp.exp(-jnp.abs(z)))
    spread = jnp.maximum(z, 0.0) + soft
    after = (
        lax.broadcasted_iota(jnp.int32, (HD, HD), 0) > lax.broadcasted_iota(jnp.int32, (HD, HD), 1)
    ).astype(jnp.bfloat16)
    strips = block_len // HD
    lanes = [slice(j * HD, (j + 1) * HD) for j in range(strips)]
    stacked = jnp.concatenate([spread[:, lane] for lane in lanes], axis=0)
    high = stacked.astype(jnp.bfloat16).astype(jnp.float32)
    middle = (stacked - high).astype(jnp.bfloat16).astype(jnp.float32)
    thirds = jnp.concatenate([stacked - high - middle, middle, high], axis=0).astype(jnp.bfloat16)
    found = jnp.dot(thirds, after, preferred_element_type=jnp.float32)
    size = count * ROWS
    found = found[: strips * size] + found[strips * size : 2 * strips * size] + found[2 * strips * size :]
    sums = jnp.zeros((size, 1), jnp.float32)
    parts = []
    for j in reversed(range(strips)):
        inner = found[j * size : (j + 1) * size]
        parts.append(inner + sums)
        sums = sums + inner[:, :1] + spread[:, j * HD : j * HD + 1]
    inside = jnp.concatenate(parts[::-1], axis=1)
    weights = jnp.exp(jnp.minimum(z, 0.0) - soft - inside).astype(jnp.bfloat16)
    for i in range(count):
        lines = slice(i * ROWS, (i + 1) * ROWS)
        totals[blocks[i]] = jnp.broadcast_to(sums[lines], (ROWS, HD))
        mixed[blocks[i]] = jnp.dot(
            weights[lines], held[i][block_len : 2 * block_len, :], preferred_element_type=jnp.float32
        )
    if final:
        carried = jnp.zeros((ROWS, HD), jnp.float32)
        mixture = jnp.zeros((ROWS, HD), jnp.float32)
        for block in reversed(range(totals.shape[0])):
            mixture = mixture + jnp.exp(-carried) * mixed[block]
            carried = carried + totals[block]
            offset_out[0, :, block * block_len : (block + 1) * block_len] = rows[block].astype(jnp.bfloat16)
        mean = jnp.mean(mixture * mixture, axis=-1, keepdims=True)
        read = (mixture * lax.rsqrt(mean + EPSILON)).astype(jnp.bfloat16)
        for g in range(QG):
            read_out[0, :, g * HD : (g + 1) * HD] = read[g : g + 1, :]
    for store in stores:
        store.wait()


def read(pieces, queries, head_bias, sp_count, block_len, values, earlier=()):
    final = bool(earlier)
    count = len(pieces)
    length = sp_count * block_len
    caches = [jax.ShapeDtypeStruct((1, 1, length, HD), jnp.bfloat16)] * 2
    partial = [jax.ShapeDtypeStruct((sp_count, ROWS, HD), jnp.float32)] * 2
    partial.append(jax.ShapeDtypeStruct((sp_count, 1, block_len), jnp.float32))
    results = [jax.ShapeDtypeStruct((1, 1, length), jnp.bfloat16), jax.ShapeDtypeStruct(queries.shape, jnp.bfloat16)]
    return pl.pallas_call(
        functools.partial(read_kernel, pieces, final),
        out_shape=caches + (results if final else partial),
        in_specs=[VMEM, SMEM] + [VMEM] * count + ([VMEM, VMEM, VMEM, ANY, ANY] if final else []),
        out_specs=[ANY, ANY] + [VMEM] * (2 if final else 3),
        scratch_shapes=([pltpu.VMEM(p.shape, p.dtype) for p in partial] if final else [])
        + [
            pltpu.VMEM((count * ROWS, block_len), jnp.float32),
            pltpu.SemaphoreType.DMA((2 * count,)),
        ],
        input_output_aliases={2 + count + 3: 0, 2 + count + 4: 1} if final else {},
        compiler_params=pltpu.CompilerParams(vmem_limit_bytes=32 * 1024 * 1024),
        cost_estimate=pl.CostEstimate(
            flops=64 * count * block_len * HD, bytes_accessed=8 * count * block_len * HD, transcendentals=0
        ),
        name="read",
    )(queries, head_bias, *(pltpu.with_memory_space_constraint(value, pltpu.VMEM) for value in values), *earlier)


def shards(layer_input, input_gain, key_weight, value_weight, stick_offsets, head_bias, queries):
    _, block_len, _ = layer_input.shape
    sp_count = lax.axis_size("sp")
    groups = sp_count // KVH

    def pairs(c, k):
        return [(z, (z // KVH + c) % groups * KVH + (z % KVH ^ k)) for z in range(sp_count)]

    args = (input_gain, key_weight, value_weight, stick_offsets)
    made, normed = project(LEAD, ORDER[0][1:], layer_input, *args, keep=True)
    made.update(project(LEAD, tuple(k for k in range(KVH) if k != ORDER[0][1]), normed, *args)[0])
    made.update(project(FOLLOW, tuple(range(KVH)), layer_input, *args)[0])
    got = {(0, 0): made[0, 0]}
    for c, k in ORDER:
        got[c, k] = lax.ppermute(made[c, k], "sp", pairs(c, k))
    early = ((0, 0),) + ORDER[:-LATE]
    late = ORDER[-LATE:]
    *caches, totals, mixed, rows = read(early, queries, head_bias, sp_count, block_len, [got[piece] for piece in early])
    return tuple(
        read(
            late,
            queries,
            head_bias,
            sp_count,
            block_len,
            [got[piece] for piece in late],
            (totals, mixed, rows, *caches),
        )
    )


def solution(mesh):
    row = P(("grp", "tp"), "sp", None)
    return jax.shard_map(
        shards,
        mesh=mesh,
        in_specs=(row, P(), P(), P(), P(None, ("grp", "tp"), "sp"), P(), row),
        out_specs=(
            P(("grp", "tp"), "sp", None, None),
            P(("grp", "tp"), "sp", None, None),
            row,
            row,
        ),
        check_vma=False,
    )
```

```python
import functools
import math

import jax
import jax.numpy as jnp
from jax import lax
from jax.experimental import pallas as pl
from jax.experimental.pallas import tpu as pltpu
from jax.sharding import PartitionSpec as P


H = 16
KVH = 4
HD = 128
QG = H // KVH
EPSILON = 1e-06
ROWS = 8
EXTRA = 8

ORDER = (
    ((2, 0), (2, 3))
    + ((1, 0), (3, 1), (1, 2), (3, 0))
    + ((2, 2), (2, 1))
    + ((1, 3), (3, 2), (1, 1), (3, 3))
    + ((0, 2), (0, 3), (0, 1))
)
LEAD = (2,)
FOLLOW = (((1, 3), 1), ((0,), 9))
CHUNKS = 3
STEP = 16
LATE = 3

ANY = pl.BlockSpec(memory_space=pltpu.HBM)
VMEM = pl.BlockSpec(memory_space=pltpu.VMEM)
SMEM = pl.BlockSpec(memory_space=pltpu.SMEM)


def split_index():
    z = lax.axis_index("sp")
    return lax.div(z, KVH), lax.rem(z, KVH), lax.axis_size("sp") // KVH


def project_kernel(classes, heads, given, keep, x_ref, gain_ref, key_ref, value_ref, offset_ref, *rest):
    count = len(classes)
    outs = rest[: count * len(heads)]
    rest = rest[count * len(heads) :]
    normed, *rest = rest
    weights, offsets, w_sems = rest[:3]
    group, member, groups = split_index()
    prompts = [lax.rem(group + c, groups) for c in classes]
    block_len = normed.shape[0] // count
    small = pltpu.make_async_copy(offset_ref, offsets, w_sems.at[2 * len(heads)])
    columns = [pl.ds(pl.multiple_of((member ^ k) * HD, HD), HD) for k in heads]
    loads = [
        pltpu.make_async_copy(ref.at[:, columns[i]], weights.at[i, :, w * HD : (w + 1) * HD], w_sems.at[2 * i + w])
        for i in range(len(heads))
        for w, ref in enumerate((key_ref, value_ref))
    ]
    if not given:
        rows, gains, x_sems = rest[3:]
        gain_load = pltpu.make_async_copy(gain_ref, gains, w_sems.at[2 * len(heads) + 1])
        gain_load.start()
        chunk = block_len // CHUNKS
        reads = [
            pltpu.make_async_copy(
                x_ref.at[prompts[n], pl.ds(i * chunk, chunk)],
                rows.at[pl.ds(n * block_len + i * chunk, chunk)],
                x_sems.at[n * CHUNKS + i],
            )
            for n in range(count)
            for i in range(CHUNKS)
        ]
        for load in reads[:CHUNKS]:
            load.start()
    for load in loads:
        load.start()
    small.start()
    if not given:
        for load in reads[CHUNKS:]:
            load.start()
        gain_load.wait()
        gain = gains[...].reshape(1, -1)
        for i, load in enumerate(reads):
            load.wait()

            def normalize(r, _, i=i):
                start = pl.multiple_of(i * chunk + r * STEP, STEP)
                wide = rows[pl.ds(start, STEP), :].astype(jnp.float32)
                mean = jnp.mean(wide * wide, axis=-1, keepdims=True)
                normed[pl.ds(start, STEP), :] = (wide * lax.rsqrt(mean + EPSILON) * gain).astype(jnp.bfloat16)
                return 0

            lax.fori_loop(0, chunk // STEP, normalize, 0, unroll=4)
    else:
        normed = x_ref
    small.wait()
    line = lax.broadcasted_iota(jnp.int32, (EXTRA, HD), 0)
    prompt = lax.broadcasted_iota(jnp.int32, (offsets.shape[1], 1), 0)
    for n in range(count):
        for i, k in enumerate(heads):
            own = offsets[member ^ k].astype(jnp.float32)
            own = jnp.sum(jnp.where(prompt == prompts[n], own, 0.0), axis=0, keepdims=True)
            extra = jnp.zeros((EXTRA, HD), jnp.float32)
            for j in range(block_len // HD):
                extra = jnp.where(line == j, own[:, j * HD : (j + 1) * HD], extra)
            outs[n * len(heads) + i][2 * block_len :, :] = extra.astype(jnp.bfloat16)
    for i in range(len(heads)):
        loads[2 * i].wait()
        loads[2 * i + 1].wait()
        product = jnp.dot(normed[...], weights[i], preferred_element_type=jnp.float32).astype(jnp.bfloat16)
        for n in range(count):
            out = outs[n * len(heads) + i]
            for w in range(2):
                out[w * block_len : (w + 1) * block_len, :] = product[
                    n * block_len : (n + 1) * block_len, w * HD : (w + 1) * HD
                ]


def project(classes, heads, source, input_gain, key_weight, value_weight, stick_offsets, keep=False):
    given = source.ndim == 2
    width = source.shape[-1]
    block_len = source.shape[-2]
    count = len(classes)
    piece = jax.ShapeDtypeStruct((2 * block_len + EXTRA, HD), jnp.bfloat16)
    normed = (count * block_len, width)
    scratch = [] if keep else [pltpu.VMEM(normed if not given else (block_len, HD), jnp.bfloat16)]
    scratch += [
        pltpu.VMEM((len(heads), width, 2 * HD), jnp.bfloat16),
        pltpu.VMEM(stick_offsets.shape, stick_offsets.dtype),
        pltpu.SemaphoreType.DMA((2 * len(heads) + 2,)),
    ]
    if not given:
        scratch += [
            pltpu.VMEM(normed, jnp.bfloat16),
            pltpu.VMEM(input_gain.shape, input_gain.dtype),
            pltpu.SemaphoreType.DMA((count * CHUNKS,)),
        ]
    made = pl.pallas_call(
        functools.partial(project_kernel, classes, heads, given, keep),
        out_shape=[piece] * (count * len(heads)) + ([jax.ShapeDtypeStruct(normed, jnp.bfloat16)] if keep else []),
        in_specs=[VMEM if given else ANY] + [ANY] * 4,
        out_specs=[VMEM] * (count * len(heads) + keep),
        scratch_shapes=scratch,
        compiler_params=pltpu.CompilerParams(vmem_limit_bytes=48 * 1024 * 1024),
        cost_estimate=pl.CostEstimate(
            flops=4 * count * len(heads) * block_len * width * HD,
            bytes_accessed=count * block_len * width * 2 + 4 * width * HD * len(heads),
            transcendentals=0,
        ),
        name="project",
    )(
        source if given else pltpu.with_memory_space_constraint(source, pltpu.HBM),
        *(
            pltpu.with_memory_space_constraint(value, pltpu.HBM)
            for value in (input_gain, key_weight, value_weight, stick_offsets)
        ),
    )
    pieces = {(c, k): made[n * len(heads) + i] for n, c in enumerate(classes) for i, k in enumerate(heads)}
    return pieces, made[-1]


def read_kernel(pieces, final, q_ref, bias_ref, *rest):
    count = len(pieces)
    held = rest[:count]
    rest = rest[count:]
    if final:
        total_in, mixed_in, row_in, _, _, key_out, value_out, offset_out, read_out, totals, mixed, rows = rest[:12]
        rest = rest[12:]
    else:
        key_out, value_out, totals, mixed, rows = rest[:5]
        rest = rest[5:]
    scores, out_sems = rest
    block_len = rows.shape[2]
    group, member, groups = split_index()
    blocks = [lax.rem(group + groups - c, groups) * KVH + (member ^ k) for c, k in pieces]
    stores = []
    for i in range(count):
        place = pl.ds(pl.multiple_of(blocks[i] * block_len, block_len), block_len)
        for w, out in enumerate((key_out, value_out)):
            store = pltpu.make_async_copy(
                held[i].at[pl.ds(w * block_len, block_len)], out.at[0, 0, place], out_sems.at[2 * i + w]
            )
            store.start()
            stores.append(store)
    line = lax.broadcasted_iota(jnp.int32, (ROWS, 1), 0)
    bias = jnp.zeros((ROWS, 1), jnp.float32)
    query = jnp.zeros((ROWS, HD), jnp.float32)
    for g in range(QG):
        bias = jnp.where(line == g, bias_ref[member * QG + g], bias)
        query = jnp.where(line == g, q_ref[0, :, g * HD : (g + 1) * HD].astype(jnp.float32), query)
    query = query.astype(jnp.bfloat16)
    if final:
        totals[...] = total_in[...]
        mixed[...] = mixed_in[...]
        rows[...] = row_in[...]
    for i in range(count):
        extra = held[i][2 * block_len :, :].astype(jnp.float32)
        offset = jnp.concatenate([extra[j : j + 1, :] for j in range(block_len // HD)], axis=1)
        rows[blocks[i]] = offset
        found = lax.dot_general(
            query, held[i][:block_len, :], (((1,), (1,)), ((), ())), preferred_element_type=jnp.float32
        )
        scores[i * ROWS : (i + 1) * ROWS, :] = found / math.sqrt(HD) + bias + offset
    z = scores[...]
    soft = jnp.log1p(jnp.exp(-jnp.abs(z)))
    spread = jnp.maximum(z, 0.0) + soft
    after = (
        lax.broadcasted_iota(jnp.int32, (HD, HD), 0) > lax.broadcasted_iota(jnp.int32, (HD, HD), 1)
    ).astype(jnp.bfloat16)
    strips = block_len // HD
    lanes = [slice(j * HD, (j + 1) * HD) for j in range(strips)]
    stacked = jnp.concatenate([spread[:, lane] for lane in lanes], axis=0)
    high = stacked.astype(jnp.bfloat16).astype(jnp.float32)
    middle = (stacked - high).astype(jnp.bfloat16).astype(jnp.float32)
    thirds = jnp.concatenate([stacked - high - middle, middle, high], axis=0).astype(jnp.bfloat16)
    found = jnp.dot(thirds, after, preferred_element_type=jnp.float32)
    size = count * ROWS
    found = found[: strips * size] + found[strips * size : 2 * strips * size] + found[2 * strips * size :]
    sums = jnp.zeros((size, 1), jnp.float32)
    parts = []
    for j in reversed(range(strips)):
        inner = found[j * size : (j + 1) * size]
        parts.append(inner + sums)
        sums = sums + inner[:, :1] + spread[:, j * HD : j * HD + 1]
    inside = jnp.concatenate(parts[::-1], axis=1)
    weights = jnp.exp(jnp.minimum(z, 0.0) - soft - inside).astype(jnp.bfloat16)
    for i in range(count):
        lines = slice(i * ROWS, (i + 1) * ROWS)
        totals[blocks[i]] = jnp.broadcast_to(sums[lines], (ROWS, HD))
        mixed[blocks[i]] = jnp.dot(
            weights[lines], held[i][block_len : 2 * block_len, :], preferred_element_type=jnp.float32
        )
    if final:
        carried = jnp.zeros((ROWS, HD), jnp.float32)
        mixture = jnp.zeros((ROWS, HD), jnp.float32)
        for block in reversed(range(totals.shape[0])):
            mixture = mixture + jnp.exp(-carried) * mixed[block]
            carried = carried + totals[block]
            offset_out[0, :, block * block_len : (block + 1) * block_len] = rows[block].astype(jnp.bfloat16)
        mean = jnp.mean(mixture * mixture, axis=-1, keepdims=True)
        read = (mixture * lax.rsqrt(mean + EPSILON)).astype(jnp.bfloat16)
        for g in range(QG):
            read_out[0, :, g * HD : (g + 1) * HD] = read[g : g + 1, :]
    for store in stores:
        store.wait()


def read(pieces, queries, head_bias, sp_count, block_len, values, earlier=()):
    final = bool(earlier)
    count = len(pieces)
    length = sp_count * block_len
    caches = [jax.ShapeDtypeStruct((1, 1, length, HD), jnp.bfloat16)] * 2
    partial = [jax.ShapeDtypeStruct((sp_count, ROWS, HD), jnp.float32)] * 2
    partial.append(jax.ShapeDtypeStruct((sp_count, 1, block_len), jnp.float32))
    results = [jax.ShapeDtypeStruct((1, 1, length), jnp.bfloat16), jax.ShapeDtypeStruct(queries.shape, jnp.bfloat16)]
    return pl.pallas_call(
        functools.partial(read_kernel, pieces, final),
        out_shape=caches + (results if final else partial),
        in_specs=[VMEM, SMEM] + [VMEM] * count + ([VMEM, VMEM, VMEM, ANY, ANY] if final else []),
        out_specs=[ANY, ANY] + [VMEM] * (2 if final else 3),
        scratch_shapes=([pltpu.VMEM(p.shape, p.dtype) for p in partial] if final else [])
        + [
            pltpu.VMEM((count * ROWS, block_len), jnp.float32),
            pltpu.SemaphoreType.DMA((2 * count,)),
        ],
        input_output_aliases={2 + count + 3: 0, 2 + count + 4: 1} if final else {},
        compiler_params=pltpu.CompilerParams(vmem_limit_bytes=32 * 1024 * 1024),
        cost_estimate=pl.CostEstimate(
            flops=64 * count * block_len * HD, bytes_accessed=8 * count * block_len * HD, transcendentals=0
        ),
        name="read",
    )(queries, head_bias, *(pltpu.with_memory_space_constraint(value, pltpu.VMEM) for value in values), *earlier)


def shards(layer_input, input_gain, key_weight, value_weight, stick_offsets, head_bias, queries):
    _, block_len, _ = layer_input.shape
    sp_count = lax.axis_size("sp")
    groups = sp_count // KVH

    def pairs(c, k):
        return [(z, (z // KVH + c) % groups * KVH + (z % KVH ^ k)) for z in range(sp_count)]

    args = (input_gain, key_weight, value_weight, stick_offsets)
    made, normed = project(LEAD, ORDER[0][1:], layer_input, *args, keep=True)
    made.update(project(LEAD, tuple(k for k in range(KVH) if k != ORDER[0][1]), normed, *args)[0])
    for classes, _ in FOLLOW:
        made.update(project(classes, tuple(range(KVH)), layer_input, *args)[0])
    got = {(0, 0): made[0, 0]}
    for c, k in ORDER:
        got[c, k] = lax.ppermute(made[c, k], "sp", pairs(c, k))
    early = ((0, 0),) + ORDER[:-LATE]
    late = ORDER[-LATE:]
    *caches, totals, mixed, rows = read(early, queries, head_bias, sp_count, block_len, [got[piece] for piece in early])
    return tuple(
        read(
            late,
            queries,
            head_bias,
            sp_count,
            block_len,
            [got[piece] for piece in late],
            (totals, mixed, rows, *caches),
        )
    )


def solution(mesh):
    row = P(("grp", "tp"), "sp", None)
    return jax.shard_map(
        shards,
        mesh=mesh,
        in_specs=(row, P(), P(), P(), P(None, ("grp", "tp"), "sp"), P(), row),
        out_specs=(
            P(("grp", "tp"), "sp", None, None),
            P(("grp", "tp"), "sp", None, None),
            row,
            row,
        ),
        check_vma=False,
    )
```
